256 devices in a mesh: sp: 64 (over z, y, core), tp: 4 (over x).
Axes of the slice: x: 4, y: 4, z: 8, core: 2. Of those that a mesh axis runs over, the one named last changes fastest.
Arguments:
- query_input: bfloat16 [32768, 1024], P('sp', 'tp'), may hold values from -6 to 6
- value_input: bfloat16 [32768, 1024], P('sp', 'tp'), may hold values from -6 to 6
- forget_ahead: bfloat16 [32768, 1024], P('sp', 'tp'), may hold values from -7.5 to 7.5
- forget_behind: bfloat16 [32768, 1024], P('sp', 'tp'), may hold values from -7.5 to 7.5
- output_gate: bfloat16 [32768, 1024], P('sp', 'tp'), may hold values from -6 to 6
- floor_ahead: float32 [1024], P('tp'), may hold values from 0.9 to 0.9999951
- floor_behind: float32 [1024], P('tp'), may hold values from 0.9 to 0.9999951
- head_gain: float32 [1024], P('tp'), may hold values from 0.1 to 1.9
- decay_jolts: float32 [8, 32768], P('tp', 'sp'), may hold values from -2.1 to 0
- residual: bfloat16 [32768, 2048], P(('sp', 'tp')), may hold values from -6 to 6
- out_weight: bfloat16 [1024, 2048], replicated, may hold values from -0.1875 to 0.1875
- norm_gain: float32 [2048], replicated, may hold values from 0.1 to 1.9
- norm_bias: float32 [2048], replicated, may hold values from -1.5 to 1.5
- expert_ids: int32 [32768, 2], P('sp'), may hold values from 0 to 63, all different within a row; in each aligned block of 128 rows (0 to 127, 128 to 255, ...) at most 8 rows name the same one
- route_scale: float32 [32768, 2], P('sp'), may hold values from 0.3 to 1.5
- expert_gate: bfloat16 [64, 2048, 512], P('sp', None, 'tp'), may hold values from -0.125 to 0.125
- expert_up: bfloat16 [64, 2048, 512], P('sp', None, 'tp'), may hold values from -0.125 to 0.125
- expert_down: bfloat16 [64, 512, 2048], P('sp', 'tp'), may hold values from -0.25 to 0.25
- shared_gate: bfloat16 [2048, 512], P(None, 'tp'), may hold values from -0.125 to 0.125
- shared_up: bfloat16 [2048, 512], P(None, 'tp'), may hold values from -0.125 to 0.125
- shared_down: bfloat16 [512, 2048], P('tp'), may hold values from -0.25 to 0.25
Outputs:
- layer_output: bfloat16 [32768, 2048], P(('sp', 'tp'))
The draws below stay inside these ranges and needn't reach their ends.
Inputs may be any that keep to these rules, and one draw needn't show every extreme that they name: `expert_ids`: A position's 2 experts differ. In each aligned block of 128 positions no expert is named by more than 8 of the block's positions, and in some block one expert is named by exactly 8; every expert is named somewhere.
All inputs are finite; a program needn't handle non-finite values.
Results may differ from the reference program's by a relative error of at most 0.015.
Values may be sent and summed in bfloat16 or wider, within the bound.
A program may use at most 128 MiB of HBM per device.

```python
import math
import jax
import jax.numpy as jnp
import numpy as np
from jax import lax

D = 2048
HEADS = 8
HEAD_DIM = 128
HG_WIDTH = 1024
BLOCK = 128
FFE = 512
FFS = 512
EXPERTS = 64
TOPK = 2
TOK_DEV = 512
ROWS = 128
TOKENS = 32768
SLICES = 4
CAP = 8
N_SP = 64
N_TP = 4


def forget_draw(key):
    noise_key, shift_key = jax.random.split(key)
    noise = jnp.clip(jax.random.normal(noise_key, (TOKENS, HG_WIDTH), jnp.float32), -6.0, 6.0)
    shifts = jax.random.uniform(shift_key, (TOKENS // TOK_DEV, 1, 1), jnp.float32, -1.5, 1.5)
    shaped = noise.reshape(TOKENS // TOK_DEV, TOK_DEV, HG_WIDTH) + shifts
    return shaped.reshape(TOKENS, HG_WIDTH).astype(jnp.bfloat16)


def draw_forget_ahead(key, part):
    return forget_draw(jax.random.fold_in(key, 101))


def draw_forget_behind(key, part):
    return forget_draw(jax.random.fold_in(key, 202))


def lower_bounds(key):
    pick_key, slow_key, fast_key, jitter_key = jax.random.split(key, 4)
    share = 0.5
    slow_heads = jax.random.uniform(pick_key, (HEADS, 1), jnp.float32) < share
    slow_gap = jnp.exp(jax.random.uniform(slow_key, (HEADS, 1), jnp.float32, jnp.log(0.2), jnp.log(1.0))) / TOKENS
    fast_gap = jnp.exp(jax.random.uniform(fast_key, (HEADS, 1), jnp.float32, jnp.log(0.02), jnp.log(0.08)))
    jitter = jnp.exp(jax.random.uniform(jitter_key, (HEADS, HEAD_DIM), jnp.float32, jnp.log(0.8), jnp.log(1.2)))
    gap_size = jnp.where(slow_heads, slow_gap, fast_gap) * jitter
    return (1.0 - gap_size).reshape(HG_WIDTH).astype(jnp.float32)


def draw_floor_ahead(key, part):
    return lower_bounds(jax.random.fold_in(key, 303))


def draw_floor_behind(key, part):
    return lower_bounds(jax.random.fold_in(key, 404))


def draw_decay_jolts(key, part):
    place_key, size_key = jax.random.split(jax.random.fold_in(key, 505))
    spots = jax.random.randint(place_key, (HEADS, 3), 0, TOKENS)
    losses = jnp.log(jax.random.uniform(size_key, (HEADS, 3), jnp.float32, 0.5, 0.8))
    head_rows = jnp.broadcast_to(jnp.arange(HEADS)[:, None], (HEADS, 3))
    return jnp.zeros((HEADS, TOKENS), jnp.float32).at[head_rows, spots].add(losses)


def steps_of(rng, shape, cuts, least, high):
    loudness, own = 1.0, jax.random.fold_in(rng, 6)
    for position, shards_of in cuts:
        heights = jnp.exp(jax.random.uniform(jax.random.fold_in(own, position), (shards_of,), jnp.float32, least / len(cuts), high / len(cuts)))
        loudness = loudness * jnp.repeat(heights, shape[position] // shards_of).reshape([-1 if axis == position else 1 for axis in range(len(shape))])
    return loudness


def shared_out(stream_key, own, number, rows, amount, top, bound, skew):
    sequence = jax.random.permutation(stream_key, amount)
    packed, common = shares(amount, rows * top, bound, skew, True), shares(amount, rows * top, bound, skew, False)
    places = jnp.arange(amount)

    def named(sizes, offset_by):
        used = int((sizes > 0).sum())
        fixed = max(1, used // 4)
        passed = fixed + (places - fixed + offset_by * (used - fixed)) % max(1, amount - fixed)
        return jnp.zeros((amount,), jnp.int32).at[sequence[jnp.where(places < fixed, places, passed)]].set(jnp.asarray(sizes, jnp.int32))

    sizes = jnp.where(number % 4 == 0, named(packed, number // 4), named(common, number - number // 4 - 1))
    mixed = jax.random.permutation(jax.random.fold_in(own, 3), amount)
    donor, sink = mixed[0:amount // 2 * 2:2], mixed[1:amount // 2 * 2:2]
    margin = jnp.minimum(sizes[donor] - 1, bound - sizes[sink]) // 2
    margin = jnp.where((donor == sequence[0]) | (sink == sequence[0]) | (sizes[sink] == 0), 0, jnp.maximum(margin, 0))
    passed = jax.random.randint(jax.random.fold_in(own, 4), (amount // 2,), 0, 1 << 20) % (margin + 1)
    sizes = sizes.at[donor].add(-passed).at[sink].add(passed)
    members = jnp.searchsorted(jnp.cumsum(sizes), jnp.arange(rows * top), side="right").astype(jnp.int32)
    listing = members.reshape(top, rows).T
    listing = listing[jax.random.permutation(jax.random.fold_in(own, 1), rows)]
    offset_by = jax.random.randint(jax.random.fold_in(own, 2), (rows, 1), 0, top)
    return jnp.take_along_axis(listing, (jnp.arange(top)[None, :] + offset_by) % top, axis=1)


def shares(amount, total, reach, slope, full):
    weights = [(1 << 20) // math.isqrt(rank ** slope) + 1 for rank in range(1, amount + 1)]
    largest = reach if full else min(reach, max(-(-total // amount), total * weights[0] // sum(weights)))
    least = 1 if total - largest >= amount - 1 else 0
    holding, rest = [largest] + [least] * (amount - 1), total - largest - least * (amount - 1)
    while rest > 0:
        candidates = [i for i in range(1, amount) if holding[i] < largest] or [i for i in range(1, amount) if holding[i] < reach]
        mass, remaining = sum([weights[i] for i in candidates]), rest
        for i in candidates:
            addition = min(reach - holding[i], max(1, remaining * weights[i] // mass), rest)
            holding[i] = holding[i] + addition
            rest = rest - addition
    return np.array(holding)


def normal_values(key, extent, deviation, bound, shards=(), kind=jnp.bfloat16):
    level = steps_of(key, extent, shards, -0.22, 0.18) if shards else 1.0
    values = jax.random.normal(key, extent, jnp.float32) * deviation * level
    return jnp.minimum(jnp.maximum(values, -bound), bound).astype(kind)


def setup_inputs(seed: int = 0) -> dict:
    key_list = jax.random.split(jax.random.key(seed), 22)
    query_input = normal_values(key_list[0], (TOKENS, HG_WIDTH), 1.0, 6.0, ((0, 64), (1, 4)))
    value_input = normal_values(key_list[1], (TOKENS, HG_WIDTH), 1.0, 6.0, ((0, 64), (1, 4)))
    forget_ahead = draw_forget_ahead(jax.random.fold_in(key_list[21], 71), 0)
    forget_behind = draw_forget_behind(jax.random.fold_in(key_list[21], 71), 0)
    output_gate = normal_values(key_list[4], (TOKENS, HG_WIDTH), 1.0, 6.0, ((0, 64), (1, 4)))
    floor_ahead = draw_floor_ahead(jax.random.fold_in(key_list[21], 71), 0)
    floor_behind = draw_floor_behind(jax.random.fold_in(key_list[21], 71), 0)
    head_gain = jnp.clip(1.0 + 0.18 * jax.random.normal(key_list[7], (HG_WIDTH,), jnp.float32), 0.1, 1.9)
    decay_jolts = draw_decay_jolts(jax.random.fold_in(key_list[21], 71), 0)
    residual = normal_values(key_list[9], (TOKENS, D), 1.0, 6.0, ((0, 256),))
    out_weight = normal_values(key_list[10], (HG_WIDTH, D), HG_WIDTH ** -0.5, 0.1875)
    norm_gain = jnp.clip(1.0 + 0.18 * jax.random.normal(key_list[11], (D,), jnp.float32), 0.1, 1.9)
    norm_bias = normal_values(key_list[12], (D,), 0.3, 1.5, (), jnp.float32)
    expert_ids_keys = jax.random.split(jax.random.fold_in(key_list[13], 1), TOKENS // ROWS)
    expert_ids_turns = jax.random.permutation(jax.random.fold_in(key_list[13], 3), TOKENS // ROWS)
    expert_ids = jax.vmap(lambda own, number: shared_out(jax.random.fold_in(key_list[13], 2), own, number, ROWS, EXPERTS, TOPK, CAP, 1))(expert_ids_keys, expert_ids_turns).reshape((TOKENS, TOPK))
    route_scale = jnp.clip(0.3 + 1.2 * jax.random.uniform(key_list[14], (TOKENS, TOPK), jnp.float32) ** steps_of(key_list[14], (TOKENS, TOPK), ((0, 64),), -0.2, 0.2), 0.3, 1.5)
    expert_gate = normal_values(key_list[15], (EXPERTS, D, FFE), D ** -0.5, 0.125, ((0, 64), (2, 4)))
    expert_up = normal_values(key_list[16], (EXPERTS, D, FFE), D ** -0.5, 0.125, ((0, 64), (2, 4)))
    expert_down = normal_values(key_list[17], (EXPERTS, FFE, D), FFE ** -0.5, 0.25, ((0, 64), (1, 4)))
    shared_gate = normal_values(key_list[18], (D, FFS), D ** -0.5, 0.125, ((1, 4),))
    shared_up = normal_values(key_list[19], (D, FFS), D ** -0.5, 0.125, ((1, 4),))
    shared_down = normal_values(key_list[20], (FFS, D), FFS ** -0.5, 0.25, ((0, 4),))
    return {"query_input": query_input, "value_input": value_input, "forget_ahead": forget_ahead, "forget_behind": forget_behind, "output_gate": output_gate, "floor_ahead": floor_ahead, "floor_behind": floor_behind, "head_gain": head_gain, "decay_jolts": decay_jolts, "residual": residual, "out_weight": out_weight, "norm_gain": norm_gain, "norm_bias": norm_bias, "expert_ids": expert_ids, "route_scale": route_scale, "expert_gate": expert_gate, "expert_up": expert_up, "expert_down": expert_down, "shared_gate": shared_gate, "shared_up": shared_up, "shared_down": shared_down}


epsilon = 1e-05
residual_scale = 2.0 ** 0.25
highest = lax.Precision.HIGHEST

def heads_first(source, head_count):
    length = source.shape[0]
    return source.astype(jnp.float32).reshape(length, head_count, -1).transpose(1, 0, 2)

def forget_terms(pre_gate, lower_bound, jolt_logs):
    forget_rate = (1.0 - lower_bound) * jax.nn.sigmoid(-pre_gate)
    return (forget_rate, jnp.log1p(-forget_rate) + jolt_logs)

def direction_terms(queries, keys_in, values, log_decay, block_len):
    head_count, length, state_width = queries.shape
    block_count = length // block_len

    def to_blocks(array):
        return array.reshape(head_count, block_count, block_len, array.shape[-1]).transpose(1, 0, 2, 3)
    query_blocks = to_blocks(queries)
    key_blocks = to_blocks(keys_in)
    value_blocks = to_blocks(values)
    cumulative = jnp.cumsum(to_blocks(log_decay), axis=2)
    middle = cumulative[:, :, block_len // 2 - 1:block_len // 2]
    block_end = cumulative[:, :, -1:]
    prefix = jnp.tril(jnp.ones((block_len, block_len), jnp.float32))
    scores = jnp.einsum('nhce,nhse->nhcs', query_blocks * jnp.exp(cumulative - middle), key_blocks * jnp.exp(middle - cumulative), precision=highest)
    within = jnp.einsum('nhcs,nhsv->nhcv', scores * prefix, value_blocks, precision=highest)
    query_start = query_blocks * jnp.exp(cumulative)
    key_end = key_blocks * jnp.exp(block_end - cumulative)
    decays = jnp.exp(block_end[:, :, 0])

    def advance(carry_state, pieces):
        query_piece, key_piece, value_piece, decay_piece = pieces
        readout = jnp.einsum('hce,hev->hcv', query_piece, carry_state, precision=highest)
        carry_state = decay_piece[..., None] * carry_state + jnp.einsum('hce,hcv->hev', key_piece, value_piece, precision=highest)
        return (carry_state, readout)
    zero_state = jnp.zeros((head_count, state_width, values.shape[-1]), jnp.float32)
    end_state, carried = lax.scan(advance, zero_state, (query_start, key_end, value_blocks, decays))
    block_out = (within + carried).transpose(1, 0, 2, 3).reshape(head_count, length, -1)
    decay_total = jnp.exp(lax.optimization_barrier(jnp.sum(log_decay, axis=1)))
    return (block_out, decay_total, end_state)

def finish_heads(summed, head_gain, gate_pre):
    head_count, length, state_width = summed.shape
    normed = summed * lax.rsqrt(lax.optimization_barrier(jnp.mean(summed * summed, axis=2, keepdims=True)) + epsilon)
    normed = normed * head_gain.reshape(head_count, 1, state_width)
    merged = normed.transpose(1, 0, 2).reshape(length, head_count * state_width)
    return (merged * jax.nn.silu(gate_pre.astype(jnp.float32))).astype(jnp.bfloat16)

def layer_norm(summed, norm_gain, norm_bias):
    centre = lax.optimization_barrier(jnp.mean(summed, axis=1, keepdims=True))
    shifted = summed - centre
    spread = lax.optimization_barrier(jnp.mean(shifted * shifted, axis=1, keepdims=True))
    return (shifted * lax.rsqrt(spread + epsilon) * norm_gain + norm_bias).astype(jnp.bfloat16)

def swiglu_sum(rows_in, gate_matrix, up_matrix, down_matrix, slice_count):
    gate_act = jnp.dot(rows_in, gate_matrix, preferred_element_type=jnp.float32)
    upward = jnp.dot(rows_in, up_matrix, preferred_element_type=jnp.float32)
    hidden = (jax.nn.silu(gate_act) * upward).astype(jnp.bfloat16)
    piece_width = hidden.shape[1] // slice_count
    running = jnp.zeros((rows_in.shape[0], down_matrix.shape[1]), jnp.float32)
    for part_index in range(slice_count):
        partial_term = jnp.dot(hidden[:, part_index * piece_width:(part_index + 1) * piece_width], down_matrix[part_index * piece_width:(part_index + 1) * piece_width], preferred_element_type=jnp.float32)
        running = running + lax.optimization_barrier(partial_term.astype(jnp.bfloat16)).astype(jnp.float32)
    return running

def slot_ranks(chosen, expert_count):
    flat_ids = chosen.reshape(-1)
    one_hot = (flat_ids[:, None] == jnp.arange(expert_count, dtype=jnp.int32)[None, :]).astype(jnp.int32)
    before = jnp.cumsum(one_hot, axis=0) - one_hot
    return lax.optimization_barrier(jnp.sum(before * one_hot, axis=1)).astype(jnp.int32)

def slot_sources(targets, top_count, slot_total):
    owners = jnp.arange(targets.shape[0], dtype=jnp.int32) // top_count
    source = jnp.zeros((slot_total,), jnp.int32).at[targets].set(owners)
    filled = jnp.zeros((slot_total,), jnp.int32).at[targets].set(1)
    return (source, filled)

def reference(query_input, value_input, forget_ahead, forget_behind, output_gate, floor_ahead, floor_behind, head_gain, decay_jolts, residual, out_weight, norm_gain, norm_bias, expert_ids, route_scale, expert_gate, expert_up, expert_down, shared_gate, shared_up, shared_down):
    head_count = decay_jolts.shape[0]
    queries = jax.nn.silu(heads_first(query_input, head_count))
    values = heads_first(value_input, head_count)
    state_width = queries.shape[2]
    jolt_logs = decay_jolts[:, :, None]
    rate_ahead, log_ahead = forget_terms(heads_first(forget_ahead, head_count), floor_ahead.reshape(head_count, 1, state_width), jolt_logs)
    rate_behind, log_behind = forget_terms(jnp.flip(heads_first(forget_behind, head_count), 1), floor_behind.reshape(head_count, 1, state_width), jnp.flip(jolt_logs, 1))
    ahead_out = direction_terms(queries, rate_ahead, values, log_ahead, BLOCK)[0]
    behind_out = direction_terms(jnp.flip(queries, 1), rate_behind, jnp.flip(values, 1), log_behind, BLOCK)[0]
    mixed_rows = finish_heads(ahead_out + jnp.flip(behind_out, 1), head_gain, output_gate)
    projected = jnp.dot(mixed_rows, out_weight, preferred_element_type=jnp.float32)
    normed_rows = layer_norm(residual_scale * residual.astype(jnp.float32) + projected, norm_gain, norm_bias)
    blocks = N_SP * N_TP
    block_ids = expert_ids.reshape(blocks, ROWS, TOPK)
    slot_rank = jax.vmap(lambda chosen: slot_ranks(chosen, EXPERTS))(block_ids)
    lane_size = blocks * CAP
    targets = (block_ids.reshape(blocks, ROWS * TOPK) * lane_size + jnp.arange(blocks, dtype=jnp.int32)[:, None] * CAP + slot_rank).reshape(-1).astype(jnp.int32)
    source, filled = slot_sources(targets, TOPK, EXPERTS * lane_size)

    def run_expert(pieces):
        gate_matrix, up_matrix, down_matrix, source_rows, filled_rows = pieces
        taken_rows = jnp.take(normed_rows, source_rows, axis=0)
        rows_in = jnp.where(filled_rows[:, None] > 0, taken_rows, jnp.zeros_like(taken_rows))
        return swiglu_sum(rows_in, gate_matrix, up_matrix, down_matrix, SLICES).astype(jnp.bfloat16)
    expert_out = lax.map(run_expert, (expert_gate, expert_up, expert_down, source.reshape(EXPERTS, lane_size), filled.reshape(EXPERTS, lane_size)))
    picked = jnp.take(expert_out.reshape(EXPERTS * lane_size, D), targets, axis=0)
    picked = picked.astype(jnp.float32).reshape(TOKENS, TOPK, D)
    routed = lax.optimization_barrier(jnp.sum(picked * route_scale[:, :, None], axis=1))
    shared = swiglu_sum(normed_rows, shared_gate, shared_up, shared_down, SLICES)
    return (residual_scale * normed_rows.astype(jnp.float32) + shared + routed).astype(jnp.bfloat16)
```

```python
import functools

import jax
import jax.numpy as jnp
from jax import lax
from jax.experimental import pallas as pl
from jax.experimental.pallas import tpu as pltpu
from jax.sharding import Mesh
from jax.sharding import PartitionSpec as P

BLOCK = 128
SP = ("sp_0", "sp_1", "sp_2")
SP_TP = ("sp_0", "sp_1", "sp_2", "tp")
MESH = pl.DeviceIdType.MESH
F32 = jnp.float32
BF16 = jnp.bfloat16

epsilon = 1e-05
residual_scale = 2.0**0.25
VMEM_LIMIT = 60 * 1024 * 1024


def dot(a, b, dims):
    return lax.dot_general(a, b, (dims, ((), ())), preferred_element_type=F32)


def split_two(value):
    high = value.astype(BF16)
    return high, (value - high.astype(F32)).astype(BF16)


def slot_picks(ids_ref, first_row, rows, slots, capacity):
    slot = lax.broadcasted_iota(jnp.int32, (rows, slots), 1)
    expert = slot // capacity
    rank_wanted = (slot % capacity).astype(F32)
    picks = [ids_ref[pl.ds(first_row, rows), k : k + 1] == expert for k in range(2)]
    named = (picks[0] | picks[1]).astype(F32)
    row = lax.broadcasted_iota(jnp.int32, (rows, rows), 0)
    col = lax.broadcasted_iota(jnp.int32, (rows, rows), 1)
    before = (col < row).astype(BF16)
    rank = dot(before, named.astype(BF16), ((1,), (0,)))
    here = rank == rank_wanted
    return [jnp.where(p & here, 1.0, 0.0).astype(BF16) for p in picks]


def mixer_kernel(
    sizes,
    q_ref, v_ref, fa_ref, fb_ref, og_ref, floor_a_ref, floor_b_ref, gain_ref, jolt_ref,
    residual_ref, weight_ref, norm_gain_ref, norm_bias_ref, ids_ref,
    normed_ref, slots_ref, picks_ref,
    res_buf, w_buf, summed, qm, km, qs, blk_state, blk_end, tot,
    sib_recv, out1, in1, out2, in2, sib_out, entering, acc, mixed, mixed_in,
    load_sem, sib_sem, s1, r1, s2, r2, sib2_sem, st, rt,
):
    nz, ny, ntp, heads, blocks, capacity = sizes
    n = nz * ny
    width = heads * 128
    part = heads * 128 // n
    z = lax.axis_index("sp_0")
    y = lax.axis_index("sp_1")
    c = lax.axis_index("sp_2")
    x = lax.axis_index("tp")
    me = z * ny + y
    sib = (z, y, 1 - c, x)

    def chip(k):
        j = lax.rem(me + k, n)
        return j, (j // ny, lax.rem(j, ny), c, x)

    def tp_peer(k):
        j = lax.rem(x + k, ntp)
        return j, (z, y, c, j)

    barrier = pltpu.get_barrier_semaphore()
    pl.semaphore_signal(barrier, inc=1, device_id=sib, device_id_type=MESH)

    def greet_chip(k, carry):
        pl.semaphore_signal(barrier, inc=1, device_id=chip(k)[1], device_id_type=MESH)
        return carry

    lax.fori_loop(1, n, greet_chip, 0)

    def greet_tp(k, carry):
        pl.semaphore_signal(barrier, inc=1, device_id=tp_peer(k)[1], device_id_type=MESH)
        return carry

    lax.fori_loop(1, ntp, greet_tp, 0)

    load_w = pltpu.make_async_copy(weight_ref, w_buf, load_sem.at[0])
    load_w.start()
    load_r = pltpu.make_async_copy(residual_ref, res_buf, load_sem.at[1])
    load_r.start()

    row_i = lax.broadcasted_iota(jnp.int32, (BLOCK, BLOCK), 0)
    col_i = lax.broadcasted_iota(jnp.int32, (BLOCK, BLOCK), 1)
    masks = (col_i <= row_i, col_i >= row_i)

    def local_block(b, carry):
        rows = pl.ds(pl.multiple_of(b * BLOCK, BLOCK), BLOCK)
        q = q_ref[rows, :].astype(F32)
        q = q / (1.0 + jnp.exp(-q))
        v = v_ref[rows, :]
        jolt = jnp.concatenate(
            [jnp.broadcast_to(jolt_ref[h : h + 1, rows], (BLOCK, BLOCK)).T for h in range(heads)],
            axis=1,
        )
        for d, (f_ref, floor_ref) in enumerate(((fa_ref, floor_a_ref), (fb_ref, floor_b_ref))):
            f = f_ref[rows, :].astype(F32)
            rate = (1.0 - floor_ref[...]) / (1.0 + jnp.exp(f))
            high, low = split_two(jnp.log1p(-rate) + jolt)
            tri = masks[d].astype(F32).astype(BF16)
            cum = dot(tri, high, ((1,), (0,))) + dot(tri, low, ((1,), (0,)))
            at_mid, at_end = (BLOCK // 2 - 1, BLOCK - 1) if d == 0 else (BLOCK // 2, 0)
            mid = cum[at_mid : at_mid + 1]
            end = cum[at_end : at_end + 1]
            q_scaled = q * jnp.exp(cum - mid)
            k_scaled = rate * jnp.exp(mid - cum)
            qm[d, rows, :] = q_scaled.astype(BF16)
            km[d, rows, :] = k_scaled.astype(BF16)
            qs[d, rows, :] = (q_scaled * jnp.exp(mid)).astype(BF16)
            k_end = (k_scaled * jnp.exp(end - mid)).astype(BF16)
            for h in range(heads):
                cols = slice(h * 128, (h + 1) * 128)
                blk_state[d, b, cols, :] = dot(v[:, cols], k_end[:, cols], ((0,), (0,)))
            blk_end[d, b] = jnp.broadcast_to(end, (8, width))
        return carry

    lax.fori_loop(0, blocks, local_block, 0)

    for d in range(2):
        order = list(range(blocks)) if d == 0 else list(reversed(range(blocks)))
        total_end = blk_end[d, order[0]]
        for b in order[1:]:
            total_end = total_end + blk_end[d, b]
        for h in range(heads):
            cols = slice(h * 128, (h + 1) * 128)
            state = blk_state[d, order[0], cols, :]
            for b in order[1:]:
                decay = jnp.exp(blk_end[d, b, 0:1, cols])
                state = decay * state + blk_state[d, b, cols, :]
            tot[d, cols, :] = state
            tot[d, width + h * 8 : width + h * 8 + 8, :] = jnp.exp(total_end[:, cols])

    pl.semaphore_wait(barrier, 1 + (n - 1) + (ntp - 1))

    to_sib = pltpu.make_async_remote_copy(
        tot.at[1 - c], sib_recv, sib_sem.at[0], sib_sem.at[1], device_id=sib, device_id_type=MESH
    )
    to_sib.start()
    to_sib.wait()

    half = n // heads
    for h in range(heads):
        cols = slice(h * 128, (h + 1) * 128)
        dec_rows = slice(width + h * 8, width + h * 8 + 8)
        own_decay = tot[c, dec_rows, :]
        sib_decay = sib_recv[dec_rows, :]
        state = sib_decay[0:1] * tot[c, cols, :] + sib_recv[cols, :]
        high, low = split_two(own_decay * sib_decay)
        dec_iota = lax.broadcasted_iota(jnp.int32, (8, 128), 0)
        decays = jnp.where(dec_iota < 4, high.astype(F32), low.astype(F32))
        message = jnp.concatenate(
            [state.reshape(half, part, 128), jnp.broadcast_to(decays[None], (half, 8, 128))], axis=1
        )
        out1[h * half : (h + 1) * half] = message.astype(BF16)
    in1[pl.ds(me, 1)] = out1[pl.ds(me, 1)]

    def first_copy(k):
        j, peer = chip(k)
        return pltpu.make_async_remote_copy(
            out1.at[j], in1.at[me], s1.at[j], r1.at[me], device_id=peer, device_id_type=MESH
        )

    def first_arrival(k):
        j, peer = chip(k)
        return pltpu.make_async_remote_copy(
            out1.at[j], in1.at[j], s1.at[j], r1.at[j], device_id=peer, device_id_type=MESH
        )

    lax.fori_loop(1, n, lambda k, s: (first_copy(k).start(), s)[1], 0)

    def inside_block(b, carry):
        rows = pl.ds(pl.multiple_of(b * BLOCK, BLOCK), BLOCK)
        v = v_ref[rows, :]
        for h in range(heads):
            cols = slice(h * 128, (h + 1) * 128)
            both = None
            for d in range(2):
                scores = dot(qm[d, rows, cols], km[d, rows, cols], ((1,), (1,)))
                kept = jnp.where(masks[d], scores, 0.0).astype(BF16)
                term = dot(kept, v[:, cols], ((1,), (0,)))
                both = term if both is None else both + term
            acc[rows, cols] = both
        return carry

    lax.fori_loop(0, blocks, inside_block, 0)

    lax.fori_loop(1, n, lambda k, s: (first_arrival(k).wait_recv(), s)[1], 0)

    def scan_step(k, run):
        j = c * (n - 1) + (1 - 2 * c) * k
        item = in1[j].astype(F32)
        decay = item[part : part + 1] + item[part + 4 : part + 5]
        out2[j] = run
        return decay * run + item[0:part]

    lax.fori_loop(0, n, scan_step, jnp.zeros((part, 128), F32))
    in2[pl.ds(me, 1)] = out2[pl.ds(me, 1)]

    def second_copy(k):
        j, peer = chip(k)
        return pltpu.make_async_remote_copy(
            out2.at[j], in2.at[me], s2.at[j], r2.at[me], device_id=peer, device_id_type=MESH
        )

    def second_arrival(k):
        j, peer = chip(k)
        return pltpu.make_async_remote_copy(
            out2.at[j], in2.at[j], s2.at[j], r2.at[j], device_id=peer, device_id_type=MESH
        )

    lax.fori_loop(1, n, lambda k, s: (second_copy(k).start(), s)[1], 0)
    lax.fori_loop(1, n, lambda k, s: (first_copy(k).wait_send(), s)[1], 0)
    lax.fori_loop(1, n, lambda k, s: (second_arrival(k).wait_recv(), s)[1], 0)

    first = in2[...].reshape(width, 128)
    for h in range(heads):
        cols = slice(h * 128, (h + 1) * 128)
        own_decay = tot[c, width + h * 8 : width + h * 8 + 1, :]
        sib_out[cols, :] = own_decay * first[cols] + tot[c, cols, :]
    back = pltpu.make_async_remote_copy(
        sib_out, entering.at[c], sib2_sem.at[0], sib2_sem.at[1], device_id=sib, device_id_type=MESH
    )
    back.start()
    entering[c] = first

    def carried(d):
        def step(k, carry):
            b = d * (blocks - 1) + (1 - 2 * d) * k
            rows = pl.ds(pl.multiple_of(b * BLOCK, BLOCK), BLOCK)
            for h in range(heads):
                cols = slice(h * 128, (h + 1) * 128)
                state = entering[d, cols, :]
                acc[rows, cols] += dot(qs[d, rows, cols], state.astype(BF16), ((1,), (1,)))
                decay = jnp.exp(blk_end[d, b, 0:1, cols])
                entering[d, cols, :] = decay * state + blk_state[d, b, cols, :]
            return carry

        lax.fori_loop(0, blocks, step, 0)

    carried(c)
    pltpu.make_async_remote_copy(
        sib_out, entering.at[1 - c], sib2_sem.at[0], sib2_sem.at[1],
        device_id=sib, device_id_type=MESH,
    ).wait_recv()
    carried(1 - c)

    local_rows = blocks * BLOCK // ntp

    def finish(j):
        rows = pl.ds(pl.multiple_of(j * local_rows, local_rows), local_rows)
        gate = og_ref[rows, :].astype(F32)
        gate = gate / (1.0 + jnp.exp(-gate))
        done = []
        for h in range(heads):
            cols = slice(h * 128, (h + 1) * 128)
            summed_h = acc[rows, cols]
            square = jnp.mean(summed_h * summed_h, axis=1, keepdims=True)
            done.append(summed_h * lax.rsqrt(square + epsilon))
        return (jnp.concatenate(done, axis=1) * gain_ref[...] * gate).astype(BF16)

    def mixed_copy(k):
        j, peer = tp_peer(k)
        return pltpu.make_async_remote_copy(
            mixed.at[j], mixed_in.at[x], st.at[j], rt.at[x], device_id=peer, device_id_type=MESH
        )

    def mixed_arrival(k):
        j, peer = tp_peer(k)
        return pltpu.make_async_remote_copy(
            mixed.at[j], mixed_in.at[j], st.at[j], rt.at[j], device_id=peer, device_id_type=MESH
        )

    def send_mixed(k, carry):
        j, _ = tp_peer(k)
        mixed[j] = finish(j)
        mixed_copy(k).start()
        return carry

    lax.fori_loop(1, ntp, send_mixed, 0)
    mixed_in[x] = finish(x)

    slots = slots_ref.shape[0]
    first_pick, second_pick = slot_picks(ids_ref, x * local_rows, local_rows, slots, capacity)
    picks_ref[0:local_rows] = first_pick
    picks_ref[local_rows : 2 * local_rows] = second_pick

    load_w.wait()
    load_r.wait()
    lax.fori_loop(1, ntp, lambda k, s: (mixed_arrival(k).wait_recv(), s)[1], 0)
    token_major = jnp.concatenate([mixed_in[p] for p in range(ntp)], axis=1)
    model = normed_ref.shape[1]
    step_cols = 512 if model % 512 == 0 else model

    def project(k, total):
        cols = pl.ds(pl.multiple_of(k * step_cols, step_cols), step_cols)
        value = residual_scale * res_buf[:, cols].astype(F32)
        value = value + dot(token_major, w_buf[:, cols], ((1,), (0,)))
        summed[:, cols] = value
        return total + jnp.sum(value, axis=1, keepdims=True)

    total = lax.fori_loop(0, model // step_cols, project, jnp.zeros((local_rows, 1), F32))
    shifted = summed[...] - total / model
    spread = jnp.mean(shifted * shifted, axis=1, keepdims=True)
    normed = shifted * lax.rsqrt(spread + epsilon) * norm_gain_ref[...] + norm_bias_ref[...]
    normed_ref[...] = normed.astype(BF16)
    both_picks = first_pick + second_pick

    def pack(k, carry):
        cols = pl.ds(pl.multiple_of(k * step_cols, step_cols), step_cols)
        slots_ref[:, cols] = dot(both_picks, normed_ref[:, cols], ((0,), (0,))).astype(BF16)
        return carry

    lax.fori_loop(0, model // step_cols, pack, 0)

    lax.fori_loop(1, n, lambda k, s: (second_copy(k).wait_send(), s)[1], 0)
    back.wait_send()
    lax.fori_loop(1, ntp, lambda k, s: (mixed_copy(k).wait_send(), s)[1], 0)


def mixer(q, v, fa, fb, og, floor_a, floor_b, gain, jolts, residual, weight, ng, nb, ids):
    nz, ny, ntp = lax.axis_size("sp_0"), lax.axis_size("sp_1"), lax.axis_size("tp")
    heads = jolts.shape[0]
    length, width = q.shape
    blocks = length // BLOCK
    local_rows, model = residual.shape
    experts = nz * ny * lax.axis_size("sp_2")
    capacity = 2 * local_rows * ids.shape[1] // experts
    slots = experts * capacity
    n = nz * ny
    part = width // n
    vmem = pl.BlockSpec(memory_space=pltpu.VMEM)
    hbm = pl.BlockSpec(memory_space=pl.ANY)
    dma = pltpu.SemaphoreType.DMA
    rows_total = width + 8 * heads
    scratch = [
        pltpu.VMEM((local_rows, model), BF16),
        pltpu.VMEM(weight.shape, BF16),
        pltpu.VMEM((local_rows, model), F32),
        pltpu.VMEM((2, length, width), BF16),
        pltpu.VMEM((2, length, width), BF16),
        pltpu.VMEM((2, length, width), BF16),
        pltpu.VMEM((2, blocks, width, 128), F32),
        pltpu.VMEM((2, blocks, 8, width), F32),
        pltpu.VMEM((2, rows_total, 128), F32),
        pltpu.VMEM((rows_total, 128), F32),
        pltpu.VMEM((n, part + 8, 128), BF16),
        pltpu.VMEM((n, part + 8, 128), BF16),
        pltpu.VMEM((n, part, 128), F32),
        pltpu.VMEM((n, part, 128), F32),
        pltpu.VMEM((width, 128), F32),
        pltpu.VMEM((2, width, 128), F32),
        pltpu.VMEM((length, width), F32),
        pltpu.VMEM((ntp, local_rows, width), BF16),
        pltpu.VMEM((ntp, local_rows, width), BF16),
        dma((2,)), dma((2,)), dma((n,)), dma((n,)), dma((n,)), dma((n,)),
        dma((2,)), dma((ntp,)), dma((ntp,)),
    ]
    return pl.pallas_call(
        functools.partial(mixer_kernel, (nz, ny, ntp, heads, blocks, capacity)),
        name="mixer",
        out_shape=[
            jax.ShapeDtypeStruct((local_rows, model), BF16),
            jax.ShapeDtypeStruct((slots, model), BF16),
            jax.ShapeDtypeStruct((2 * local_rows, slots), BF16),
        ],
        in_specs=[vmem] * 9 + [hbm, hbm] + [vmem] * 3,
        out_specs=[vmem, vmem, vmem],
        scratch_shapes=scratch,
        compiler_params=pltpu.CompilerParams(
            collective_id=0, has_side_effects=True, vmem_limit_bytes=VMEM_LIMIT
        ),
        cost_estimate=pl.CostEstimate(
            flops=20_000_000_000, bytes_accessed=10_000_000, transcendentals=0
        ),
    )(
        q, v, fa, fb, og, floor_a[None], floor_b[None], gain[None], jolts,
        residual, weight, ng[None], nb[None], ids,
    )


def ffn_kernel(pieces, rows_ref, *refs):
    weights = refs[: 3 * pieces]
    out_ref = refs[3 * pieces]
    gate_buf, up_buf, down_buf, hidden, sem = refs[3 * pieces + 1 :]
    piece = gate_buf.shape[2]
    copies = []
    for p in range(pieces):
        gate, up, down = weights[3 * p : 3 * p + 3]
        copies.append((
            pltpu.make_async_copy(gate, gate_buf.at[p], sem.at[p, 0]),
            pltpu.make_async_copy(up, up_buf.at[p], sem.at[p, 1]),
            pltpu.make_async_copy(down, down_buf.at[pl.ds(p * piece, piece)], sem.at[p, 2]),
        ))
    for trio in copies:
        for copy in trio:
            copy.start()
    rows = rows_ref[...]
    for p in range(pieces):
        copies[p][0].wait()
        copies[p][1].wait()
        both = dot(rows, jnp.concatenate([gate_buf[p], up_buf[p]], axis=1), ((1,), (0,)))
        gate_act, upward = both[:, :piece], both[:, piece:]
        act = gate_act / (1.0 + jnp.exp(-gate_act)) * upward
        hidden[:, p * piece : (p + 1) * piece] = act.astype(BF16)
    for p in range(pieces):
        copies[p][2].wait()
    model = out_ref.shape[1]
    step_cols = 512 if model % 512 == 0 else model

    def down_step(k, carry):
        cols = pl.ds(pl.multiple_of(k * step_cols, step_cols), step_cols)
        out_ref[:, cols] = dot(hidden[...], down_buf[:, cols], ((1,), (0,))).astype(BF16)
        return carry

    lax.fori_loop(0, model // step_cols, down_step, 0)


def ffn(rows, weights, name):
    pieces = len(weights)
    model, piece = weights[0][0].shape
    vmem = pl.BlockSpec(memory_space=pltpu.VMEM)
    hbm = pl.BlockSpec(memory_space=pl.ANY)
    flat = [w for trio in weights for w in trio]
    return pl.pallas_call(
        functools.partial(ffn_kernel, pieces),
        name=name,
        out_shape=jax.ShapeDtypeStruct(rows.shape, BF16),
        in_specs=[vmem] + [hbm] * len(flat),
        out_specs=vmem,
        scratch_shapes=[
            pltpu.VMEM((pieces, model, piece), BF16),
            pltpu.VMEM((pieces, model, piece), BF16),
            pltpu.VMEM((pieces * piece, model), BF16),
            pltpu.VMEM((rows.shape[0], pieces * piece), BF16),
            pltpu.SemaphoreType.DMA((pieces, 3)),
        ],
        compiler_params=pltpu.CompilerParams(vmem_limit_bytes=VMEM_LIMIT),
        cost_estimate=pl.CostEstimate(
            flops=6 * rows.shape[0] * model * piece * pieces,
            bytes_accessed=6 * model * piece * pieces, transcendentals=0,
        ),
    )(rows, *flat)


def combine_kernel(back_ref, normed_ref, shared_ref, picks_ref, scale_ref, out_ref):
    local_rows, model = out_ref.shape
    x = lax.axis_index("tp")
    scale = [scale_ref[pl.ds(x * local_rows, local_rows), k : k + 1] for k in range(2)]
    step_cols = 512 if model % 512 == 0 else model

    def step(k, carry):
        cols = pl.ds(pl.multiple_of(k * step_cols, step_cols), step_cols)
        both = dot(picks_ref[...], back_ref[:, cols], ((1,), (0,)))
        routed = scale[0] * both[:local_rows] + scale[1] * both[local_rows:]
        value = residual_scale * normed_ref[:, cols].astype(F32) + shared_ref[:, cols].astype(F32)
        out_ref[:, cols] = (value + routed).astype(BF16)
        return carry

    lax.fori_loop(0, model // step_cols, step, 0)


def combine(back, normed, shared, picks, scale):
    vmem = pl.BlockSpec(memory_space=pltpu.VMEM)
    return pl.pallas_call(
        combine_kernel,
        name="combine",
        out_shape=jax.ShapeDtypeStruct(normed.shape, BF16),
        in_specs=[vmem] * 5,
        out_specs=vmem,
        compiler_params=pltpu.CompilerParams(vmem_limit_bytes=VMEM_LIMIT),
        cost_estimate=pl.CostEstimate(
            flops=2 * picks.shape[0] * picks.shape[1] * normed.shape[1],
            bytes_accessed=back.size * 2, transcendentals=0,
        ),
    )(back, normed, shared, picks, scale)


def shift(values, by):
    count = lax.axis_size("tp")
    ring = [(i, (i + by) % count) for i in range(count)]
    return [lax.ppermute(v, "tp", ring) for v in values]


def near_pieces(trio):
    return [trio, shift(trio, 1), shift(trio, -1)]


def far_piece(near):
    own, left, right = near
    gate, down = shift((left[0], left[2]), 1)
    (up,) = shift((right[1],), -1)
    return [gate, up, down]


def local(
    query_input, value_input, forget_ahead, forget_behind, output_gate, floor_ahead, floor_behind,
    head_gain, decay_jolts, residual, out_weight, norm_gain, norm_bias, expert_ids, route_scale,
    expert_gate, expert_up, expert_down, shared_gate, shared_up, shared_down,
):
    expert = near_pieces([expert_gate[0], expert_up[0], expert_down[0]])
    normed, slots, picks = mixer(
        query_input, value_input, forget_ahead, forget_behind, output_gate, floor_ahead,
        floor_behind, head_gain, decay_jolts, residual, out_weight, norm_gain, norm_bias,
        expert_ids,
    )
    arrived = lax.all_to_all(
        slots.reshape(lax.axis_size(SP), -1, slots.shape[1]), SP, 0, 0, tiled=True
    )
    expert = expert + [far_piece(expert)]
    shared_gate, _ = lax.optimization_barrier((shared_gate, normed))
    shared_up, _ = lax.optimization_barrier((shared_up, normed))
    shared_down, _ = lax.optimization_barrier((shared_down, normed))
    shared = near_pieces([shared_gate, shared_up, shared_down])
    shared = shared + [far_piece(shared)]
    routed = ffn(arrived.reshape(-1, slots.shape[1]), expert, "routed")
    came_back = lax.all_to_all(
        routed.reshape(lax.axis_size(SP), -1, slots.shape[1]), SP, 0, 0, tiled=True
    )
    shared_out = ffn(normed, shared, "shared")
    return combine(
        came_back.reshape(-1, slots.shape[1]), normed, shared_out, picks, route_scale
    )


def solution(mesh):
    split = Mesh(mesh.devices.reshape(8, 4, 2, mesh.shape["tp"]), ("sp_0", "sp_1", "sp_2", "tp"))
    in_specs = (
        P(SP, "tp"),
        P(SP, "tp"),
        P(SP, "tp"),
        P(SP, "tp"),
        P(SP, "tp"),
        P("tp"),
        P("tp"),
        P("tp"),
        P("tp", SP),
        P(SP_TP, None),
        P(),
        P(),
        P(),
        P(SP, None),
        P(SP, None),
        P(SP, None, "tp"),
        P(SP, None, "tp"),
        P(SP, "tp", None),
        P(None, "tp"),
        P(None, "tp"),
        P("tp", None),
    )
    out_specs = P(SP_TP, None)
    return jax.shard_map(local, mesh=split, in_specs=in_specs, out_specs=out_specs, check_vma=False)
```
